32 devices in a mesh: sp: 8 (over z, y), tp: 4 (over x, core).
Axes of the slice: x: 2, y: 2, z: 4, core: 2. Of those that a mesh axis runs over, the one named last changes fastest.
Arguments:
- query_proj: bfloat16 [8192, 2048], P('sp', 'tp'), may hold values from -6 to 6
- key_proj: bfloat16 [8192, 2048], P('sp', 'tp'), may hold values from -6 to 6
- value_proj: bfloat16 [8192, 4096], P('sp', 'tp'), may hold values from -6 to 6
- gate_proj: bfloat16 [8192, 4096], P('sp', 'tp'), may hold values from -6 to 6
- log_decay: float32 [8192, 8], P('sp', 'tp'), may hold values from -0.75 to 0, as said below
- residual: bfloat16 [8192, 2048], P('sp'), may hold values from -4 to 4
- out_weight: bfloat16 [4096, 2048], P('tp'), may hold values from -0.09375 to 0.09375
- norm_gain: float32 [2, 2048], replicated, may hold values from 0.1 to 1.9
- norm_bias: float32 [2, 2048], replicated, may hold values from -1.5 to 1.5
- up_gate: bfloat16 [2048, 5632], P('sp', 'tp'), may hold values from -0.125 to 0.125
- up_value: bfloat16 [2048, 5632], P('sp', 'tp'), may hold values from -0.125 to 0.125
- conv_weight: float32 [2, 3, 5632], P(None, None, 'tp'), may hold values from -3 to 3
- conv_bias: float32 [2, 5632], P(None, 'tp'), may hold values from -1.5 to 1.5
- down_weight: bfloat16 [5632, 2048], P('tp', 'sp'), may hold values from -0.078125 to 0.078125
Outputs:
- layer_output: bfloat16 [8192, 2048], P(('sp', 'tp'))
The draws below stay inside these ranges and needn't reach their ends.
Inputs may be any that keep to these rules, and one draw needn't show every extreme that they name: `log_decay`: all entries are negative.
All inputs are finite; a program needn't handle non-finite values.
Results may differ from the reference program's by a relative error of at most 0.023.
Values may be sent and summed in bfloat16 or wider, within the bound.
A program may use at most 128 MiB of HBM per device.

```python
import math
import jax
import jax.numpy as jnp
from jax import lax

D = 2048
RETENTION_HEADS = 8
DK = 256
DV = 512
FF = 5632
BLOCK = 256
TOK_DEV = 1024
SEQUENCE_TOKENS = 8192
N_TP = 4


def draw_log_decay(key, part):
    random_keys = jax.random.split(jax.random.fold_in(key, 71), 7)
    fast_limit = 5
    quick_decay_heads = jax.random.randint(random_keys[0], (RETENTION_HEADS,), 0, 10) < fast_limit
    fast_span = jax.random.uniform(random_keys[1], (RETENTION_HEADS,), jnp.float32, 30.0, 50.0)
    slow_rate = -0.2 / SEQUENCE_TOKENS * jax.random.uniform(random_keys[2], (RETENTION_HEADS,), jnp.float32, 0.5, 1.0)
    decay_base_rate = jnp.where(quick_decay_heads, -math.log(10.0) / fast_span, slow_rate)
    device_count = SEQUENCE_TOKENS // TOK_DEV
    replica_multiplier = jnp.exp(jax.random.uniform(random_keys[3], (device_count, RETENTION_HEADS), jnp.float32, math.log(0.5), math.log(2.0)))
    replica_multiplier = jnp.repeat(replica_multiplier, TOK_DEV, axis=0)
    jitter_amount = jax.random.uniform(random_keys[4], (SEQUENCE_TOKENS, RETENTION_HEADS), jnp.float32, 0.5, 1.5)
    spike_positions = jax.random.randint(random_keys[5], (2, RETENTION_HEADS), 0, SEQUENCE_TOKENS)
    spike_lengths = jax.random.uniform(random_keys[6], (2, RETENTION_HEADS), jnp.float32, math.log(0.5), math.log(0.8))
    position_slots = jnp.arange(SEQUENCE_TOKENS)[:, None]
    spike_events = jnp.where(position_slots == spike_positions[0][None, :], spike_lengths[0][None, :], 0.0)
    spike_events = spike_events + jnp.where(position_slots == spike_positions[1][None, :], spike_lengths[1][None, :], 0.0)
    spike_events = jnp.where(quick_decay_heads[None, :], 0.0, spike_events)
    return (decay_base_rate[None, :] * replica_multiplier * jitter_amount + spike_events).astype(jnp.float32)


def shard_levels(rng, extent, cuts, least, largest):
    def one(position, parts):
        steps = jax.random.uniform(jax.random.fold_in(jax.random.fold_in(rng, 6), position), (parts,), jnp.float32, least / len(cuts), largest / len(cuts))
        return jnp.repeat(jnp.exp(steps), extent[position] // parts).reshape((-1,) + (1,) * (len(extent) - position - 1))

    loudness = one(*cuts[0])
    for cut in cuts[1:]:
        loudness = loudness * one(*cut)
    return loudness


def normal_values(own_key, dims, deviation, limit, cuts=(), held_as=jnp.bfloat16):
    values = jax.random.normal(own_key, dims, jnp.float32) * deviation
    if len(cuts) > 0:
        values = shard_levels(own_key, dims, cuts, -0.22, 0.18) * values
    return jnp.clip(values, min=-limit, max=limit).astype(held_as)


def setup_inputs(seed: int = 0) -> dict:
    splits = jax.random.split(jax.random.key(seed), 15)
    query_proj = normal_values(splits[0], (SEQUENCE_TOKENS, RETENTION_HEADS * DK), 1.0, 6.0, ((0, 8), (1, 4)))
    key_proj = normal_values(splits[1], (SEQUENCE_TOKENS, RETENTION_HEADS * DK), 1.0, 6.0, ((0, 8), (1, 4)))
    value_proj = normal_values(splits[2], (SEQUENCE_TOKENS, RETENTION_HEADS * DV), 1.0, 6.0, ((0, 8), (1, 4)))
    gate_proj = normal_values(splits[3], (SEQUENCE_TOKENS, RETENTION_HEADS * DV), 1.0, 6.0, ((0, 8), (1, 4)))
    log_decay = draw_log_decay(jax.random.fold_in(splits[14], 71), 0)
    residual = normal_values(splits[5], (SEQUENCE_TOKENS, D), 0.5, 4.0, ((0, 8),))
    out_weight = normal_values(splits[6], (RETENTION_HEADS * DV, D), (RETENTION_HEADS * DV) ** -0.5, 0.09375, ((0, 4),))
    norm_gain = jnp.clip(1.0 + 0.18 * jax.random.normal(splits[7], (2, D), jnp.float32), 0.1, 1.9)
    norm_bias = normal_values(splits[8], (2, D), 0.3, 1.5, (), jnp.float32)
    up_gate = normal_values(splits[9], (D, FF), D ** -0.5, 0.125, ((0, 8), (1, 4)))
    up_value = normal_values(splits[10], (D, FF), D ** -0.5, 0.125, ((0, 8), (1, 4)))
    conv_weight = normal_values(splits[11], (2, 3, FF), 0.577, 3.0, ((2, 4),), jnp.float32)
    conv_bias = normal_values(splits[12], (2, FF), 0.3, 1.5, ((1, 4),), jnp.float32)
    down_weight = normal_values(splits[13], (FF, D), FF ** -0.5, 0.078125, ((0, 4), (1, 8)))
    return dict(query_proj=query_proj, key_proj=key_proj, value_proj=value_proj, gate_proj=gate_proj, log_decay=log_decay, residual=residual, out_weight=out_weight, norm_gain=norm_gain, norm_bias=norm_bias, up_gate=up_gate, up_value=up_value, conv_weight=conv_weight, conv_bias=conv_bias, down_weight=down_weight)


alpha_scale = 8.0 ** 0.25
rope_base = 10000.0
tiny_stabilizer = 1e-05

def rotate(vectors, positions):
    head_width = vectors.shape[-1]
    half_width = head_width // 2
    inverse_freq = rope_base ** (-2.0 * jnp.arange(half_width, dtype=jnp.float32) / head_width)
    angles = positions[:, None] * inverse_freq[None, :]
    cosine = jnp.cos(angles)[:, None, :]
    sine_part = jnp.sin(angles)[:, None, :]
    front = vectors[..., :half_width]
    second = vectors[..., half_width:]
    return jnp.concatenate([front * cosine - second * sine_part, front * sine_part + second * cosine], axis=-1)

def layer_norm(values, gain, shift):
    average = values.mean(-1, keepdims=True)
    spread = jnp.square(values - average).mean(-1, keepdims=True)
    return (values - average) * lax.rsqrt(spread + tiny_stabilizer) * gain + shift

def rounded(values):
    return lax.optimization_barrier(values.astype(jnp.bfloat16)).astype(jnp.float32)

def block_parts(query_tile, lookup_piece, payload_piece, log_blk):
    cum_log = jnp.cumsum(log_blk, axis=0)
    cum_heads = cum_log.T
    log_gap = cum_heads[:, :, None] - cum_heads[:, None, :]
    offsets = jnp.arange(log_blk.shape[0])
    causal = (offsets[:, None] >= offsets[None, :])[None]
    weight = jnp.where(causal, jnp.exp(jnp.where(causal, log_gap, 0.0)), 0.0)
    score_matrix = jnp.einsum('jka,ska->kjs', query_tile.astype(jnp.float32), lookup_piece.astype(jnp.float32))
    segment_scaling = (score_matrix * weight).astype(jnp.bfloat16)
    within = jnp.einsum('htm,mhe->the', segment_scaling.astype(jnp.float32), payload_piece.astype(jnp.float32))
    block_total = cum_log[-1]
    to_end = jnp.exp(block_total[None, :] - cum_log)
    faded_lookup_vector = rounded(lookup_piece.astype(jnp.float32) * to_end[:, :, None])
    summand_term = jnp.einsum('ajo,ajd->jod', faded_lookup_vector, payload_piece.astype(jnp.float32), precision=lax.Precision.HIGHEST)
    scaled_query = rounded(query_tile.astype(jnp.float32) * jnp.exp(cum_log)[:, :, None])
    return (within, scaled_query, summand_term, jnp.exp(block_total))

def grouped_product(left, right, group_count):
    group_width = left.shape[1] // group_count
    left_groups = left.reshape(left.shape[0], group_count, group_width).transpose(1, 0, 2)
    right_groups = right.reshape(group_count, group_width, right.shape[1])

    def add_group(total, pieces):
        term = jnp.dot(pieces[0], pieces[1], preferred_element_type=jnp.float32).astype(jnp.bfloat16)
        return (total + term.astype(jnp.float32), None)
    blank_sum = jnp.zeros((left.shape[0], right.shape[1]), jnp.float32)
    total, _ = lax.scan(add_group, blank_sum, (left_groups, right_groups))
    return total

def causal_conv(rows, taps, shift):
    padded = jnp.pad(rows.astype(jnp.float32), ((2, 0), (0, 0)))
    length = rows.shape[0]
    result = shift[None, :] + padded[0:length] * taps[0]
    result = result + padded[1:length + 1] * taps[1]
    return result + padded[2:length + 2] * taps[2]

def reference(query_proj, key_proj, value_proj, gate_proj, log_decay, residual, out_weight, norm_gain, norm_bias, up_gate, up_value, conv_weight, conv_bias, down_weight):
    length = query_proj.shape[0]
    positions = jnp.arange(length).astype(jnp.float32)
    query_rot = rotate(query_proj.astype(jnp.float32).reshape(length, RETENTION_HEADS, DK), positions).astype(jnp.bfloat16)
    key_rot = (rotate(key_proj.astype(jnp.float32).reshape(length, RETENTION_HEADS, DK), positions) * DK ** (-0.5)).astype(jnp.bfloat16)
    block_count = length // BLOCK
    asking_segments = query_rot.reshape(block_count, BLOCK, RETENTION_HEADS, DK)
    key_blocks = key_rot.reshape(block_count, BLOCK, RETENTION_HEADS, DK)
    value_blocks = value_proj.reshape(block_count, BLOCK, RETENTION_HEADS, DV)
    log_blocks = log_decay.reshape(block_count, BLOCK, RETENTION_HEADS)

    def advance(carry_state, pieces):
        within, scaled_query, summand_term, block_decay = block_parts(*pieces)
        carried = jnp.einsum('thd,hde->the', scaled_query, rounded(carry_state), precision=lax.Precision.HIGHEST)
        return (block_decay[:, None, None] * carry_state + summand_term, within + carried)
    start_state = jnp.zeros((RETENTION_HEADS, DK, DV), jnp.float32)
    _, mixed_heads = lax.scan(advance, start_state, (asking_segments, key_blocks, value_blocks, log_blocks))
    mixed_heads = mixed_heads.reshape(length, RETENTION_HEADS, DV)
    average = mixed_heads.mean(-1, keepdims=True)
    spread = jnp.square(mixed_heads - average).mean(-1, keepdims=True)
    standardized_rows = (mixed_heads - average) * lax.rsqrt(spread + tiny_stabilizer)
    gate_heads = gate_proj.astype(jnp.float32).reshape(length, RETENTION_HEADS, DV)
    gated_rows = (jax.nn.silu(gate_heads) * standardized_rows).astype(jnp.bfloat16).reshape(length, RETENTION_HEADS * DV)
    attended = grouped_product(gated_rows, out_weight, N_TP)
    normed_rows = layer_norm(alpha_scale * residual.astype(jnp.float32) + attended, norm_gain[0], norm_bias[0]).astype(jnp.bfloat16)
    gate_up = jnp.dot(normed_rows, up_gate, preferred_element_type=jnp.float32).astype(jnp.bfloat16)
    value_up = jnp.dot(normed_rows, up_value, preferred_element_type=jnp.float32).astype(jnp.bfloat16)
    gate_conv = causal_conv(gate_up, conv_weight[0], conv_bias[0])
    value_conv = causal_conv(value_up, conv_weight[1], conv_bias[1])
    activated = (jax.nn.gelu(gate_conv) * value_conv).astype(jnp.bfloat16)
    ffn_out = grouped_product(activated, down_weight, N_TP)
    return layer_norm(alpha_scale * normed_rows.astype(jnp.float32) + ffn_out, norm_gain[1], norm_bias[1]).astype(jnp.bfloat16)
```

```python
import jax
import jax.numpy as jnp
from jax import lax
from jax.experimental import pallas as pl
from jax.experimental.pallas import tpu as pltpu
from jax.sharding import PartitionSpec as P

BLOCK = 256


alpha_scale = 8.0**0.25
rope_base = 10000.0
tiny_stabilizer = 1e-05


def permuted(x, axis, target):
    return lax.ppermute(x, axis, [(i, target(i)) for i in range(lax.axis_size(axis))])


def passed_along(x, axis, by):
    length = lax.axis_size(axis)
    pairs = [(i, i + by) for i in range(length) if 0 <= i + by < length]
    return lax.ppermute(x, axis, pairs)


def carried_in(decay, state):
    heads, keys, values = state.shape
    before_decay, before = jnp.ones_like(decay), jnp.zeros_like(state)
    by = 1
    while by < lax.axis_size("sp"):
        tail = jnp.broadcast_to(decay[:, None, None], (heads, 8, values))
        packed = jnp.concatenate([state, tail], axis=1).astype(jnp.bfloat16)
        packed = passed_along(packed, "sp", by).astype(jnp.float32)
        got, got_decay = packed[:, :keys], packed[:, keys, 0]
        before = before + before_decay[:, None, None] * got
        before_decay = before_decay * got_decay
        state = state + decay[:, None, None] * got
        decay = decay * got_decay
        by *= 2
    return before


def layout():
    tp, sp = lax.axis_size("tp"), lax.axis_size("sp")
    cores = 2 if tp % 2 == 0 else 1
    lines = tp // cores
    ny = lines if sp % lines == 0 else 1
    return cores, lines, ny, sp // ny


def along_z(x, ny, nz):
    return permuted(x, "sp", lambda i: (i // ny + 1) % nz * ny + i % ny)


def along_y(x, ny):
    return permuted(x, "sp", lambda i: i // ny * ny + (i % ny + 1) % ny)


def spread(piece, ny):
    row = [piece]
    for _ in range(ny - 1):
        row.append(along_y(row[-1], ny))
    return row


def tied(stage, *arrays):
    return lax.optimization_barrier((stage, *arrays))


class Gather:
    def __init__(self, piece, ny, nz, rows_first=False):
        self.ny, self.left, self.rows_first = ny, nz - 1, rows_first
        self.slots = spread(piece, ny)
        self.fresh = list(self.slots)
        self.next = None

    def send(self):
        if self.left and self.next is None:
            source = self.fresh if self.rows_first else self.fresh[:1]
            nz = lax.axis_size("sp") // self.ny
            self.next = [along_z(piece, self.ny, nz) for piece in source]
            self.left -= 1

    def land(self, stage):
        kept, extra = len(self.fresh), self.next or []
        stage, *arrived = tied(stage, *self.fresh, *extra)
        self.slots[len(self.slots) - kept :] = arrived[:kept]
        if self.next is not None:
            self.take(arrived[kept:])
        return stage

    def take(self, landed):
        self.fresh = landed if self.rows_first else spread(landed[0], self.ny)
        self.slots += self.fresh
        self.next = None

    def land_about(self, stage, work):
        kept, extra = len(self.fresh), self.next or []
        stage, *arrived = tied(stage, *self.fresh, *extra)
        self.slots[len(self.slots) - kept :] = arrived[:kept]
        stage, *landed = tied(work(stage), *arrived[kept:])
        if self.next is not None:
            self.take(landed)
        return stage

    def all(self):
        while self.left or self.next is not None:
            self.send()
            self.take(self.next)
        return self.slots


def slot_sources(ny, nz):
    place = lax.axis_index("sp")
    z, y = place // ny, place % ny
    return jnp.stack([(z - a) % nz * ny + (y - b) % ny for a in range(nz) for b in range(ny)])


def up_kernel(sources, x_ref, *refs):
    out_ref, pieces = refs[-1], refs[:-1]
    total = None
    for s, piece in enumerate(pieces):
        depth = piece.shape[1]
        columns = pl.ds(pl.multiple_of(sources[s] * depth, depth), depth)
        term = jnp.dot(x_ref[:, columns], piece[0], preferred_element_type=jnp.float32)
        total = term if total is None else total + term
    out_ref[0] = total.astype(out_ref.dtype)


def up_product(rows, slots, sources):
    count, width = rows.shape
    halves, depth, hidden = slots[0].shape
    tile = count // 2
    return pl.pallas_call(
        up_kernel,
        out_shape=jax.ShapeDtypeStruct((halves, count, hidden), jnp.bfloat16),
        grid_spec=pltpu.PrefetchScalarGridSpec(
            num_scalar_prefetch=1,
            grid=(halves, count // tile),
            in_specs=[pl.BlockSpec((tile, width), lambda g, m, _: (m, 0))]
            + [pl.BlockSpec((1, depth, hidden), lambda g, m, _: (g, 0, 0))] * len(slots),
            out_specs=pl.BlockSpec((1, tile, hidden), lambda g, m, _: (g, m, 0)),
        ),
        compiler_params=pltpu.CompilerParams(vmem_limit_bytes=56 * 2**20),
        cost_estimate=pl.CostEstimate(
            flops=2 * halves * count * width * hidden,
            bytes_accessed=2 * (count * width + halves * hidden * (width + count)),
            transcendentals=0,
        ),
    )(sources, rows, *slots)


def down_kernel(sources, act_ref, *refs):
    out_ref, pieces = refs[-1], refs[:-1]
    half = len(pieces) // 2
    split = pieces[0].shape[0]
    for s in range(half):
        depth = pieces[s].shape[1]
        columns = pl.ds(pl.multiple_of(sources[s] * depth, depth), depth)
        total = jnp.dot(act_ref[:, :split], pieces[s][...], preferred_element_type=jnp.float32)
        total += jnp.dot(
            act_ref[:, split:], pieces[half + s][...], preferred_element_type=jnp.float32
        )
        out_ref[:, columns] = total.astype(out_ref.dtype)


def down_product(act, first, second, sources):
    count, hidden = act.shape
    width = first[0].shape[1] * len(first)
    tile = count // 2
    whole = [pl.BlockSpec(p.shape, lambda m, _: (0, 0)) for p in (*first, *second)]
    return pl.pallas_call(
        down_kernel,
        out_shape=jax.ShapeDtypeStruct((count, width), jnp.bfloat16),
        grid_spec=pltpu.PrefetchScalarGridSpec(
            num_scalar_prefetch=1,
            grid=(count // tile,),
            in_specs=[pl.BlockSpec((tile, hidden), lambda m, _: (m, 0))] + whole,
            out_specs=pl.BlockSpec((tile, width), lambda m, _: (m, 0)),
        ),
        compiler_params=pltpu.CompilerParams(vmem_limit_bytes=56 * 2**20),
        cost_estimate=pl.CostEstimate(
            flops=2 * count * width * hidden,
            bytes_accessed=2 * (count * width + hidden * (width + count)),
            transcendentals=0,
        ),
    )(sources, act, *first, *second)


def scattered_sum(partial, cores, lines, after=()):
    rows, width = partial.shape
    own = rows // (cores * lines)
    place = lax.axis_index("tp")
    x, core = place // cores, place % cores
    parts = partial.reshape(lines, cores, own, width)
    total = lax.dynamic_index_in_dim(parts, core, 1, False)
    for c in range(1, cores):
        away = lax.dynamic_index_in_dim(parts, (core + c) % cores, 1, False)
        away = permuted(away, "tp", lambda i: i // cores * cores + (i % cores + c) % cores)
        total = total.astype(jnp.float32) + away.astype(jnp.float32)
    total, *after = tied(total.astype(jnp.bfloat16), *after)
    result = lax.dynamic_index_in_dim(total, x, 0, False).astype(jnp.float32)
    for d in range(1, lines):
        away = lax.dynamic_index_in_dim(total, (x + d) % lines, 0, False)
        away = permuted(away, "tp", lambda i: (i // cores + d) % lines * cores + i % cores)
        result = result + away.astype(jnp.float32)
    return (result, *after)


def gathered_rows(own, cores, lines):
    count, width = own.shape
    place = lax.axis_index("tp")
    x, core = place // cores, place % cores
    column = jnp.zeros((lines, count, width), own.dtype)
    column = lax.dynamic_update_index_in_dim(column, own, x, 0)
    for d in range(1, lines):
        got = permuted(own, "tp", lambda i: (i // cores + d) % lines * cores + i % cores)
        column = lax.dynamic_update_index_in_dim(column, got, (x - d) % lines, 0)
    whole = jnp.zeros((lines, cores, count, width), own.dtype)
    whole = lax.dynamic_update_index_in_dim(whole, column, core, 1)
    for c in range(1, cores):
        got = permuted(column, "tp", lambda i: i // cores * cores + (i % cores + c) % cores)
        whole = lax.dynamic_update_index_in_dim(whole, got, (core - c) % cores, 1)
    return whole.reshape(lines * cores * count, width)


def rotate(vectors, positions):
    head_width = vectors.shape[-1]
    half_width = head_width // 2
    inverse_freq = rope_base ** (-2.0 * jnp.arange(half_width, dtype=jnp.float32) / head_width)
    angles = positions[:, None] * inverse_freq[None, :]
    cosine = jnp.cos(angles)[:, None, :]
    sine_part = jnp.sin(angles)[:, None, :]
    front = vectors[..., :half_width]
    second = vectors[..., half_width:]
    return jnp.concatenate(
        [front * cosine - second * sine_part, front * sine_part + second * cosine], axis=-1
    )


def layer_norm(values, gain, shift):
    average = values.mean(-1, keepdims=True)
    spread = jnp.square(values - average).mean(-1, keepdims=True)
    return (values - average) * lax.rsqrt(spread + tiny_stabilizer) * gain + shift


def block_parts(query_tile, lookup_piece, payload_piece, log_blk):
    cum_log = jnp.cumsum(log_blk, axis=0)
    cum_heads = cum_log.T
    log_gap = cum_heads[:, :, None] - cum_heads[:, None, :]
    offsets = jnp.arange(log_blk.shape[0])
    causal = (offsets[:, None] >= offsets[None, :])[None]
    weight = jnp.where(causal, jnp.exp(jnp.where(causal, log_gap, 0.0)), 0.0)
    score_matrix = jnp.einsum(
        "jka,ska->kjs", query_tile, lookup_piece, preferred_element_type=jnp.float32
    )
    segment_scaling = (score_matrix * weight).astype(jnp.bfloat16)
    within = jnp.einsum(
        "htm,mhe->the", segment_scaling, payload_piece, preferred_element_type=jnp.float32
    )
    block_total = cum_log[-1]
    to_end = jnp.exp(block_total[None, :] - cum_log)
    faded_lookup_vector = (lookup_piece.astype(jnp.float32) * to_end[:, :, None]).astype(
        jnp.bfloat16
    )
    summand_term = jnp.einsum(
        "ajo,ajd->jod", faded_lookup_vector, payload_piece, preferred_element_type=jnp.float32
    )
    scaled_query = (query_tile.astype(jnp.float32) * jnp.exp(cum_log)[:, :, None]).astype(
        jnp.bfloat16
    )
    return (within, scaled_query, summand_term, jnp.exp(block_total))


def causal_conv(rows, edge_rows, taps, shift):
    padded = jnp.concatenate([edge_rows, rows], axis=0).astype(jnp.float32)
    length = rows.shape[0]
    result = shift[None, :] + padded[0:length] * taps[0]
    result = result + padded[1 : length + 1] * taps[1]
    return result + padded[2 : length + 2] * taps[2]


def shards(
    query_proj,
    key_proj,
    value_proj,
    gate_proj,
    log_decay,
    residual,
    out_weight,
    norm_gain,
    norm_bias,
    up_gate,
    up_value,
    conv_weight,
    conv_bias,
    down_weight,
):
    cores, lines, ny, nz = layout()
    ups = Gather(jnp.stack([up_gate, up_value]), ny, nz)
    ups.send()
    split = down_weight.shape[0] // 256 * 128
    sources = slot_sources(ny, nz)
    tok_rows = query_proj.shape[0]
    head_count = log_decay.shape[1]
    key_width = query_proj.shape[1] // head_count
    value_width = value_proj.shape[1] // head_count
    positions = (lax.axis_index("sp") * tok_rows + jnp.arange(tok_rows)).astype(jnp.float32)
    query_rot = rotate(
        query_proj.astype(jnp.float32).reshape(tok_rows, head_count, key_width), positions
    ).astype(jnp.bfloat16)
    key_rot = (
        rotate(key_proj.astype(jnp.float32).reshape(tok_rows, head_count, key_width), positions)
        * key_width ** (-0.5)
    ).astype(jnp.bfloat16)
    block_count = tok_rows // BLOCK
    asking_segments = query_rot.reshape(block_count, BLOCK, head_count, key_width)
    key_blocks = key_rot.reshape(block_count, BLOCK, head_count, key_width)
    value_blocks = value_proj.reshape(block_count, BLOCK, head_count, value_width)
    log_blocks = log_decay.reshape(block_count, BLOCK, head_count)
    within, scaled_query, summand_term, block_decay = jax.vmap(block_parts)(
        asking_segments, key_blocks, value_blocks, log_blocks
    )

    def absorb(carry_state, pieces):
        return (pieces[1][:, None, None] * carry_state + pieces[0], None)

    zero_state = jnp.zeros((head_count, key_width, value_width), jnp.float32)
    own_state, _ = lax.scan(absorb, zero_state, (summand_term, block_decay))
    own_decay = jnp.prod(block_decay, axis=0)
    incoming = ups.land_about(own_state, lambda state: carried_in(own_decay, state))
    ups.send()

    def advance(carry_state, pieces):
        carried = jnp.einsum(
            "thd,hde->the",
            pieces[0],
            carry_state.astype(jnp.bfloat16),
            preferred_element_type=jnp.float32,
        )
        return (pieces[2][:, None, None] * carry_state + pieces[1], carried)

    _, carried = lax.scan(advance, incoming, (scaled_query, summand_term, block_decay))
    carried = ups.land(carried)
    ups.send()
    mixed_heads = (within + carried).reshape(tok_rows, head_count, value_width)
    average = mixed_heads.mean(-1, keepdims=True)
    spread = jnp.square(mixed_heads - average).mean(-1, keepdims=True)
    standardized_rows = (mixed_heads - average) * lax.rsqrt(spread + tiny_stabilizer)
    gate_heads = gate_proj.astype(jnp.float32).reshape(tok_rows, head_count, value_width)
    gated_rows = (
        (jax.nn.silu(gate_heads) * standardized_rows)
        .astype(jnp.bfloat16)
        .reshape(tok_rows, head_count * value_width)
    )
    own_count = tok_rows // lax.axis_size("tp")
    gated_rows = ups.land(gated_rows)
    places = cores * lines

    def half_of(array, h):
        kept = array.shape[0] // (2 * places)
        return array.reshape(places, 2, kept, array.shape[1])[:, h].reshape(places * kept, -1)

    partials = [
        jnp.dot(half_of(gated_rows, h), out_weight, preferred_element_type=jnp.float32).astype(
            jnp.bfloat16
        )
        for h in range(2)
    ]
    partials[1], first_piece, second_piece = tied(
        partials[1], down_weight[:split], down_weight[split:]
    )
    first = Gather(first_piece, ny, nz)
    first.send()
    second = Gather(second_piece, ny, nz, rows_first=True)
    second.send()
    attended = [scattered_sum(p, cores, lines)[0] for p in partials]
    attended[1] = second.land(first.land(ups.land(attended[1])))
    first.send()
    second.send()
    own_input = lax.dynamic_slice_in_dim(residual, lax.axis_index("tp") * own_count, own_count, 0)
    normed_halves, gathered = [], []
    for h, own_half in enumerate(jnp.split(own_input, 2)):
        normed_halves.append(
            layer_norm(
                alpha_scale * own_half.astype(jnp.float32) + attended[h], norm_gain[0], norm_bias[0]
            ).astype(jnp.bfloat16)
        )
        gathered.append(gathered_rows(normed_halves[h], cores, lines))
    gathered[1] = second.land(first.land(gathered[1]))
    width = gathered[0].shape[1]
    whole_rows = jnp.stack([g.reshape(places, -1, width) for g in gathered], axis=1)
    whole_rows = whole_rows.reshape(tok_rows, width)
    ups = up_product(whole_rows, ups.all(), sources)
    edges = passed_along(ups[:, tok_rows - 2 :], "sp", 1)
    gate_conv = causal_conv(ups[0], edges[0], conv_weight[0], conv_bias[0])
    value_conv = causal_conv(ups[1], edges[1], conv_weight[1], conv_bias[1])
    activated = (jax.nn.gelu(gate_conv) * value_conv).astype(jnp.bfloat16)
    first_slots, second_slots = first.all(), second.all()
    results, waiting = [], [half_of(activated, h) for h in range(2)]
    while waiting:
        partial_ffn = down_product(waiting[0], first_slots, second_slots, sources)
        ffn_out, *waiting = scattered_sum(partial_ffn, cores, lines, waiting[1:])
        h = len(results)
        results.append(
            layer_norm(
                alpha_scale * normed_halves[h].astype(jnp.float32) + ffn_out,
                norm_gain[1],
                norm_bias[1],
            ).astype(jnp.bfloat16)
        )
    return jnp.concatenate(results)


def solution(mesh):
    placed = (
        P("sp", "tp"),
        P("sp", "tp"),
        P("sp", "tp"),
        P("sp", "tp"),
        P("sp", "tp"),
        P("sp", None),
        P("tp", None),
        P(),
        P(),
        P("sp", "tp"),
        P("sp", "tp"),
        P(None, None, "tp"),
        P(None, "tp"),
        P("tp", "sp"),
    )
    return jax.shard_map(
        shards, mesh=mesh, in_specs=placed, out_specs=P(("sp", "tp"), None), check_vma=False
    )
```
